32 devices in a mesh: sp: 16 (over z, y, x), tp: 2 (over core).
Axes of the slice: x: 2, y: 2, z: 4, core: 2. Of those that a mesh axis runs over, the one named last changes fastest.
Arguments:
- tokens: bfloat16 [2048, 2048], P('sp'), may hold values from -6 to 6
- norm_gain: float32 [2048], replicated, may hold values from 0.1 to 1.9
- conv_value_weight: bfloat16 [2048, 1024], P('sp', 'tp'), may hold values from -0.125 to 0.125
- conv_gate_weight: bfloat16 [2048, 1024], P('sp', 'tp'), may hold values from -0.125 to 0.125
- conv_kernel: float32 [31, 1024], P(None, 'tp'), may hold values from -10 to 10
- conv_bias: float32 [1024], P('tp'), may hold values from -4 to 4
- channel_gain: float32 [1024], P('tp'), may hold values from 0.1 to 1.9
- query_weight: bfloat16 [2048, 2048], P('sp', 'tp'), may hold values from -0.125 to 0.125
- key_weight: bfloat16 [2048, 2048], P('sp', 'tp'), may hold values from -0.125 to 0.125
- value_weight: bfloat16 [2048, 4096], P('sp', 'tp'), may hold values from -0.125 to 0.125
- gate_weight: bfloat16 [2048, 32], replicated, may hold values from -0.125 to 0.125
- gate_offset: float32 [2, 2, 8, 2048], P(None, None, 'tp', 'sp'), may hold values from -110 to 160, as said below
- start_memory: float32 [2, 8, 512, 256], P(None, 'tp'), may hold values from -0.375 to 0.375
- start_norm: float32 [2, 8, 256], P(None, 'tp'), may hold values from -0.375 to 0.375
- start_level: float32 [2, 8], P(None, 'tp'), may hold values from 2 to 5
- cell_gain: float32 [4096], P('tp'), may hold values from 0.1 to 1.9
- out_conv_weight: bfloat16 [2048, 1024], P('sp', 'tp'), may hold values from -0.25 to 0.25
- out_cell_weight: bfloat16 [2048, 4096], P('sp', 'tp'), may hold values from -0.09375 to 0.09375
Outputs:
- mixed: bfloat16 [2048, 2048], P(('sp', 'tp'))
The draws below stay inside these ranges and needn't reach their ends.
Inputs may be any that keep to these rules, and one draw needn't show every extreme that they name: `gate_offset`: added to the gate pre-activations; index 0 of the second dimension is the input gate, index 1 the forget gate.
All inputs are finite; a program needn't handle non-finite values.
Results may differ from the reference program's by a relative error of at most 0.017.
Values may be sent and summed in bfloat16 or wider, within the bound.
A program may use at most 192 MiB of HBM per device.

```python
import math
import jax
import jax.numpy as jnp
from jax import lax

D = 2048
CONV_W = 1024
MEMORY_GROUPS = 8
KEY_DIM = 256
VALUE_DIM = 512
KERNEL = 31
BLOCK = 128
TOK_DEV = 128
STEP_COUNT = 2048
N_TP = 2


def draw_conv_kernel(key, part):
    base_key, rough_key = jax.random.split(jax.random.fold_in(key, 11))
    channel = jnp.arange(CONV_W, dtype=jnp.float32) / CONV_W
    roughness = jnp.exp(jax.random.uniform(rough_key, (CONV_W,), minval=-0.5, maxval=0.5))
    channel_scale = jnp.exp(math.log(8.0) * channel)
    entries = jnp.clip(jax.random.normal(base_key, (KERNEL, CONV_W)), -4.0, 4.0)
    return (entries * channel_scale * roughness / math.sqrt(KERNEL)).astype(jnp.float32)


def draw_gate_offset(key, part):
    frequency_seed, permute_seed, surge_seed, feature_seed = jax.random.split(jax.random.fold_in(key, 23), 4)
    step_index = jnp.arange(STEP_COUNT)
    device_block = step_index // TOK_DEV
    device_count = STEP_COUNT // TOK_DEV
    device_rate = jnp.exp(jax.random.uniform(frequency_seed, (2, MEMORY_GROUPS, device_count), minval=math.log(0.4), maxval=math.log(2.5)))
    rate_here = jnp.take(device_rate, device_block, axis=2)
    order_keys = jax.random.split(permute_seed, 2)
    head_rank = jnp.stack([jax.random.permutation(order_keys[0], MEMORY_GROUPS), jax.random.permutation(order_keys[1], MEMORY_GROUPS)])
    fast_count = MEMORY_GROUPS // 2
    slow_level = jnp.log(2.0 * STEP_COUNT / rate_here)
    input_part = jnp.clip(jax.random.normal(feature_seed, (2, MEMORY_GROUPS, STEP_COUNT)), -4.0, 4.0)
    fast_head = (head_rank < fast_count)[:, :, None]
    surge_index = jax.random.randint(surge_seed, (2, MEMORY_GROUPS, 2), 0, STEP_COUNT)
    surge_flags = jnp.any(step_index[None, None, None, :] == surge_index[:, :, :, None], axis=2)
    decay_fraction = jnp.where(fast_head, 3.2, slow_level)
    decay_fraction = jnp.where(surge_flags, 0.5, decay_fraction)
    return jnp.stack([input_part, decay_fraction], axis=1).astype(jnp.float32)


def steps_of(stream_key, dims, pieces, smallest, largest):
    def one(dim, shards_of):
        heights = jax.random.uniform(jax.random.fold_in(jax.random.fold_in(stream_key, 6), dim), (shards_of,), jnp.float32, smallest / len(pieces), largest / len(pieces))
        return jnp.repeat(jnp.exp(heights), dims[dim] // shards_of).reshape((-1,) + (1,) * (len(dims) - dim - 1))

    gain = one(*pieces[0])
    for cut in pieces[1:]:
        gain = gain * one(*cut)
    return gain


def centred(stream_key, extent, scale, bound, cuts=(), kind=jnp.bfloat16):
    gain = steps_of(stream_key, extent, cuts, -0.22, 0.18) if cuts else 1.0
    values = jax.random.normal(stream_key, extent, jnp.float32) * scale * gain
    return jnp.minimum(jnp.maximum(values, -bound), bound).astype(kind)


def setup_inputs(seed: int = 0) -> dict:
    seeds = jax.random.split(jax.random.key(seed), 19)
    tokens = centred(seeds[0], (STEP_COUNT, D), 1.0, 6.0, ((0, 16),))
    norm_gain = jnp.clip(1.0 + 0.18 * jax.random.normal(seeds[1], (D,), jnp.float32), 0.1, 1.9)
    conv_value_weight = centred(seeds[2], (D, CONV_W), D ** -0.5, 0.125, ((0, 16), (1, 2)))
    conv_gate_weight = centred(seeds[3], (D, CONV_W), D ** -0.5, 0.125, ((0, 16), (1, 2)))
    conv_kernel = draw_conv_kernel(jax.random.fold_in(seeds[18], 71), 0)
    conv_bias = centred(seeds[5], (CONV_W,), 1.0, 4.0, ((0, 2),), jnp.float32)
    channel_gain = jnp.clip(1.0 + 0.18 * jax.random.normal(seeds[6], (CONV_W,), jnp.float32), 0.1, 1.9)
    query_weight = centred(seeds[7], (D, MEMORY_GROUPS * KEY_DIM), D ** -0.5, 0.125, ((0, 16), (1, 2)))
    key_weight = centred(seeds[8], (D, MEMORY_GROUPS * KEY_DIM), D ** -0.5, 0.125, ((0, 16), (1, 2)))
    value_weight = centred(seeds[9], (D, MEMORY_GROUPS * VALUE_DIM), D ** -0.5, 0.125, ((0, 16), (1, 2)))
    gate_weight = centred(seeds[10], (D, 4 * MEMORY_GROUPS), D ** -0.5, 0.125)
    gate_offset = draw_gate_offset(jax.random.fold_in(seeds[18], 71), 0)
    start_memory = centred(seeds[12], (2, MEMORY_GROUPS, VALUE_DIM, KEY_DIM), KEY_DIM ** -0.5, 0.375, ((1, 2),), jnp.float32)
    start_norm = centred(seeds[13], (2, MEMORY_GROUPS, KEY_DIM), KEY_DIM ** -0.5, 0.375, ((1, 2),), jnp.float32)
    start_level = jnp.clip(2.0 + 3.0 * jax.random.uniform(seeds[14], (2, MEMORY_GROUPS), jnp.float32) ** steps_of(seeds[14], (2, MEMORY_GROUPS), ((1, 2),), -0.2, 0.2), 2.0, 5.0)
    cell_gain = jnp.clip(1.0 + 0.18 * jax.random.normal(seeds[15], (MEMORY_GROUPS * VALUE_DIM,), jnp.float32), 0.1, 1.9)
    out_conv_weight = centred(seeds[16], (D, CONV_W), (CONV_W // 2) ** -0.5, 0.25, ((0, 16), (1, 2)))
    out_cell_weight = centred(seeds[17], (D, MEMORY_GROUPS * VALUE_DIM), (MEMORY_GROUPS * VALUE_DIM) ** -0.5, 0.09375, ((0, 16), (1, 2)))
    return {"tokens": tokens, "norm_gain": norm_gain, "conv_value_weight": conv_value_weight, "conv_gate_weight": conv_gate_weight, "conv_kernel": conv_kernel, "conv_bias": conv_bias, "channel_gain": channel_gain, "query_weight": query_weight, "key_weight": key_weight, "value_weight": value_weight, "gate_weight": gate_weight, "gate_offset": gate_offset, "start_memory": start_memory, "start_norm": start_norm, "start_level": start_level, "cell_gain": cell_gain, "out_conv_weight": out_conv_weight, "out_cell_weight": out_cell_weight}


EPS = 1e-06
HIGHEST = lax.Precision.HIGHEST

def back_to_wide(values):
    return lax.optimization_barrier(values.astype(jnp.bfloat16)).astype(jnp.float32)

def block_step(carried, inputs):
    memory, normer, run_level = carried
    queries, key_rows, value_rows, in_gate, log_forget = inputs
    length = queries.shape[0]
    lower_mask = jnp.arange(length)[:, None] >= jnp.arange(length)[None, :]
    cumulative = jnp.cumsum(log_forget)
    decay_table = jnp.where(lower_mask, cumulative[:, None] - cumulative[None, :] + in_gate[None, :], -jnp.inf)
    carried_level = cumulative + run_level
    top_level = jnp.maximum(carried_level, lax.optimization_barrier(jnp.max(decay_table, axis=1)))
    carry_weight = jnp.exp(carried_level - top_level)
    scores = jnp.dot(queries, key_rows.T, precision=HIGHEST) * jnp.exp(decay_table - top_level[:, None])
    numerator = jnp.dot(scores, value_rows, precision=HIGHEST) + carry_weight[:, None] * jnp.dot(queries, memory.T, precision=HIGHEST)
    denominator = lax.optimization_barrier(jnp.sum(scores, axis=1)) + carry_weight * jnp.dot(queries, normer, precision=HIGHEST)
    outputs = numerator / jnp.maximum(jnp.abs(denominator), 1.0)[:, None]
    block_total = cumulative[-1]
    tail_level = block_total - cumulative + in_gate
    new_level = jnp.maximum(block_total + run_level, jnp.max(tail_level))
    old_weight = jnp.exp(block_total + run_level - new_level)
    new_weight = jnp.exp(tail_level - new_level)
    memory = old_weight * memory + jnp.dot((value_rows * new_weight[:, None]).T, key_rows, precision=HIGHEST)
    normer = old_weight * normer + jnp.dot(new_weight, key_rows, precision=HIGHEST)
    return ((memory, normer, new_level), outputs)

def run_cell(queries, key_rows, value_rows, in_gate, log_forget, memory, normer, run_level):
    blocks = queries.shape[0] // BLOCK

    def to_blocks(values):
        return values.reshape((blocks, BLOCK) + values.shape[1:])
    final_state, outputs = lax.scan(block_step, (memory, normer, run_level), tuple((to_blocks(values) for values in (queries, key_rows, value_rows, in_gate, log_forget))))
    return outputs.reshape(queries.shape[0], value_rows.shape[1])

def head_outputs(inputs):
    queries, key_rows, value_rows, in_gate, log_forget, memory, normer, run_level = inputs
    forward = run_cell(queries, key_rows, value_rows, in_gate[0], log_forget[0], memory[0], normer[0], run_level[0])
    backward = run_cell(queries[::-1], key_rows[::-1], value_rows[::-1], in_gate[1, ::-1], log_forget[1, ::-1], memory[1], normer[1], run_level[1])[::-1]
    both_ways = forward + backward
    return both_ways * lax.rsqrt(lax.optimization_barrier(jnp.mean(both_ways * both_ways, axis=1, keepdims=True)) + EPS)

def reference(tokens, norm_gain, conv_value_weight, conv_gate_weight, conv_kernel, conv_bias, channel_gain, query_weight, key_weight, value_weight, gate_weight, gate_offset, start_memory, start_norm, start_level, cell_gain, out_conv_weight, out_cell_weight):
    features = tokens.astype(jnp.float32)
    normed = (features * lax.rsqrt(lax.optimization_barrier(jnp.mean(features * features, axis=1, keepdims=True)) + EPS) * norm_gain).astype(jnp.bfloat16)

    def project(weight):
        return jnp.dot(normed, weight, preferred_element_type=jnp.float32)
    conv_value = project(conv_value_weight).astype(jnp.bfloat16)
    conv_gate = project(conv_gate_weight).astype(jnp.bfloat16)
    gated_rows = (conv_value.astype(jnp.float32) * jax.nn.sigmoid(conv_gate.astype(jnp.float32))).astype(jnp.bfloat16)
    half_reach = KERNEL // 2
    padded = jnp.pad(gated_rows.astype(jnp.float32), ((half_reach, half_reach), (0, 0)))
    conv_sum = conv_bias + sum((conv_kernel[offset] * padded[offset:offset + STEP_COUNT] for offset in range(KERNEL)))
    channel_mean = lax.optimization_barrier(jnp.mean(conv_sum, axis=1, keepdims=True))
    channel_var = lax.optimization_barrier(jnp.mean(conv_sum * conv_sum, axis=1, keepdims=True)) - channel_mean * channel_mean
    conv_out = jax.nn.silu((conv_sum - channel_mean) * lax.rsqrt(channel_var + EPS) * channel_gain).astype(jnp.bfloat16)

    def split_heads(flat_rows, head_width):
        return jnp.transpose(back_to_wide(flat_rows).reshape(STEP_COUNT, MEMORY_GROUPS, head_width), (1, 0, 2))
    queries = split_heads(project(query_weight), KEY_DIM)
    key_rows = split_heads(project(key_weight), KEY_DIM) * KEY_DIM ** (-0.5)
    value_rows = split_heads(project(value_weight), VALUE_DIM)
    gate_pre = project(gate_weight).reshape(STEP_COUNT, 2, 2, MEMORY_GROUPS)
    gate_pre = jnp.transpose(gate_pre, (1, 2, 3, 0)) + gate_offset
    in_gate = jnp.transpose(gate_pre[:, 0], (1, 0, 2))
    log_forget = jnp.transpose(jax.nn.log_sigmoid(gate_pre[:, 1]), (1, 0, 2))
    cells = lax.map(head_outputs, (queries, key_rows, value_rows, in_gate, log_forget, jnp.transpose(start_memory, (1, 0, 2, 3)), jnp.transpose(start_norm, (1, 0, 2)), jnp.transpose(start_level, (1, 0))))
    cell_out = (jnp.transpose(cells, (1, 0, 2)).reshape(STEP_COUNT, MEMORY_GROUPS * VALUE_DIM) * cell_gain).astype(jnp.bfloat16)
    conv_groups = conv_out.reshape(STEP_COUNT, N_TP, CONV_W // N_TP)
    cell_groups = cell_out.reshape(STEP_COUNT, N_TP, MEMORY_GROUPS * VALUE_DIM // N_TP)
    conv_weights = out_conv_weight.reshape(D, N_TP, CONV_W // N_TP)
    cell_weights = out_cell_weight.reshape(D, N_TP, MEMORY_GROUPS * VALUE_DIM // N_TP)
    mixed_sum = jnp.zeros((STEP_COUNT, D), jnp.float32)
    for group in range(N_TP):
        partial_value = jnp.einsum('tc,dc->td', conv_groups[:, group], conv_weights[:, group], preferred_element_type=jnp.float32) + jnp.einsum('tc,dc->td', cell_groups[:, group], cell_weights[:, group], preferred_element_type=jnp.float32)
        mixed_sum = mixed_sum + lax.optimization_barrier(partial_value.astype(jnp.bfloat16)).astype(jnp.float32)
    return mixed_sum.astype(jnp.bfloat16)
```

```python
import functools

import jax
import jax.numpy as jnp
from jax import lax
from jax.experimental import pallas as pl
from jax.experimental.pallas import tpu as pltpu
from jax.sharding import Mesh, PartitionSpec as P

EPS = 1e-06
HIGHEST = lax.Precision.HIGHEST
CHUNK = 128
OUTER, HEAD, TP = "outer", "head", "tp"


def running_sum(values):
    lead, length = values.shape[:-1], values.shape[-1]
    chunk = min(CHUNK, length)
    count = length // chunk
    blocks = values.reshape(lead + (count, chunk))
    inside = (jnp.arange(chunk)[:, None] <= jnp.arange(chunk)[None, :]).astype(jnp.float32)
    before = (jnp.arange(count)[:, None] < jnp.arange(count)[None, :]).astype(jnp.float32)
    local = jnp.einsum("...cs,st->...ct", blocks, inside, precision=HIGHEST)
    start = jnp.einsum("...c,cd->...d", local[..., -1], before, precision=HIGHEST)
    return (local + start[..., None]).reshape(values.shape)


def own_columns(weight, parts, part):
    return lax.dynamic_slice_in_dim(
        weight, part * (weight.shape[-1] // parts), weight.shape[-1] // parts, weight.ndim - 1
    )


def by_head(weights, parts):
    return jnp.concatenate(
        [
            jnp.transpose(w.reshape(w.shape[0], parts, w.shape[1] // parts), (1, 0, 2))
            for w in weights
        ],
        axis=2,
    )


def spread(blocks):
    mine = lax.all_to_all(blocks, HEAD, 0, 0, tiled=True)
    return mine.reshape(mine.shape[0] * mine.shape[1], mine.shape[2])


MESH = pl.DeviceIdType.MESH


def exchange_kernel(groups, parts, *refs):
    normed, gates, key, value, conv_value, conv_gate, query, out_conv, out_cell = refs[:9]
    rows, all_gates, key_value, others, outs = refs[9:14]
    send, recv, local = refs[14:]
    group, part = lax.axis_index(OUTER), lax.axis_index(HEAD)
    depth = key.shape[0]
    away = [(g, p) for g in range(groups) for p in range(parts) if (g, p) != (0, 0)]

    def device(step):
        return {
            OUTER: lax.rem(group + step[0], groups),
            HEAD: lax.rem(part + step[1], parts),
        }

    barrier = pltpu.get_barrier_semaphore()
    for step in away:
        pl.semaphore_signal(barrier, inc=1, device_id=device(step), device_id_type=MESH)
    pl.semaphore_wait(barrier, len(away))

    place = group * parts + part
    deep = pl.ds(pl.multiple_of(place * depth, depth), depth)
    flat = pl.ds(pl.multiple_of(part * depth, depth), depth)

    def pieces(target, step, stage):
        def columns(ref):
            width = ref.shape[1] // parts
            return ref.at[:, pl.ds(pl.multiple_of(target * width, width), width)]

        def packed(refs_in, ref_out, at):
            column = 0
            found = []
            for ref in refs_in:
                width = ref.shape[1] // parts
                found.append((columns(ref), ref_out.at[at, pl.ds(column, width)]))
                column += width
            return found

        if stage == 0:
            return [(normed, rows.at[flat])] if step[0] == 0 else []
        if stage == 1:
            return packed((key, value), key_value, deep) + [(gates, all_gates.at[place])]
        if stage == 2:
            return packed((conv_value, conv_gate, query), others, deep)
        return packed((out_conv, out_cell), outs, flat) if step[0] == 0 else []

    copies = []
    kept = []
    for stage in range(4):
        for step in away:
            for source, target in pieces(lax.rem(part + step[1], parts), step, stage):
                copies.append(
                    pltpu.make_async_remote_copy(
                        src_ref=source,
                        dst_ref=target,
                        send_sem=send.at[len(copies)],
                        recv_sem=recv.at[len(copies)],
                        device_id=device(step),
                        device_id_type=MESH,
                    )
                )
                copies[-1].start()
        for source, target in pieces(part, (0, 0), stage):
            kept.append(pltpu.make_async_copy(source, target, local.at[len(kept)]))
            kept[-1].start()
    for copy in kept:
        copy.wait()
    for copy in copies:
        copy.wait()


def exchange(groups, parts, *arrays):
    normed, gates, key, value, conv_value, conv_gate, query, out_conv, out_cell = arrays
    depth, count = key.shape[0], groups * parts

    def made(height, *weights):
        width = sum(w.shape[1] // parts for w in weights)
        return jax.ShapeDtypeStruct((height, width), key.dtype)

    shapes = (
        jax.ShapeDtypeStruct((parts * normed.shape[0], normed.shape[1]), normed.dtype),
        jax.ShapeDtypeStruct((count,) + gates.shape, gates.dtype),
        made(count * depth, key, value),
        made(count * depth, conv_value, conv_gate, query),
        made(parts * depth, out_conv, out_cell),
    )
    many = 6 * (count - 1) + 3 * (parts - 1)
    return pl.pallas_call(
        functools.partial(exchange_kernel, groups, parts),
        out_shape=shapes,
        in_specs=[pl.BlockSpec(memory_space=pltpu.VMEM)] * len(arrays),
        out_specs=[pl.BlockSpec(memory_space=pl.ANY)] * len(shapes),
        scratch_shapes=[
            pltpu.SemaphoreType.DMA((many,)),
            pltpu.SemaphoreType.DMA((many,)),
            pltpu.SemaphoreType.DMA((9,)),
        ],
        compiler_params=pltpu.CompilerParams(collective_id=1, has_side_effects=True),
        name="exchange",
    )(*arrays)


def scatter_kernel(parts, partial, out, met, sums, landed, send, recv, far_send, far_recv):
    part, side = lax.axis_index(HEAD), lax.axis_index(TP)
    other = 1 - side

    def peer(step):
        return {HEAD: lax.rem(part + step, parts)}

    barrier = pltpu.get_barrier_semaphore()
    pl.semaphore_signal(barrier, inc=1, device_id={TP: other}, device_id_type=MESH)
    for step in range(1, parts):
        pl.semaphore_signal(barrier, inc=1, device_id=peer(step), device_id_type=MESH)
    pl.semaphore_wait(barrier, parts)

    near = []
    order = list(range(1, parts)) + [0]
    for step in order:
        near.append(
            pltpu.make_async_remote_copy(
                src_ref=partial.at[lax.rem(part + step, parts), other],
                dst_ref=met.at[step],
                send_sem=send.at[step],
                recv_sem=recv.at[step],
                device_id={TP: other},
                device_id_type=MESH,
            )
        )
        near[-1].start()
    far = []
    for step, copy in zip(order, near):
        copy.wait()
        total = partial[lax.rem(part + step, parts), side].astype(jnp.float32) + met[step].astype(
            jnp.float32
        )
        sums[step] = total.astype(sums.dtype)
        if step:
            far.append(
                pltpu.make_async_remote_copy(
                    src_ref=sums.at[step],
                    dst_ref=landed.at[step],
                    send_sem=far_send.at[step],
                    recv_sem=far_recv.at[step],
                    device_id=peer(step),
                    device_id_type=MESH,
                )
            )
            far[-1].start()
    total = sums[0].astype(jnp.float32)
    for step, copy in zip(order, far):
        copy.wait()
        total = total + landed[step].astype(jnp.float32)
    out[...] = total.astype(out.dtype)


def scatter(parts, partial):
    sides = 2
    height, width = partial.shape[0] // (parts * sides), partial.shape[1]
    blocks = partial.reshape(parts, sides, height, width)
    stack = pltpu.VMEM((parts, height, width), partial.dtype)
    return pl.pallas_call(
        functools.partial(scatter_kernel, parts),
        out_shape=jax.ShapeDtypeStruct((height, width), partial.dtype),
        in_specs=[pl.BlockSpec(memory_space=pltpu.VMEM)],
        out_specs=pl.BlockSpec(memory_space=pltpu.VMEM),
        scratch_shapes=[stack, stack, stack] + [pltpu.SemaphoreType.DMA((parts,))] * 4,
        compiler_params=pltpu.CompilerParams(collective_id=2, has_side_effects=True),
        name="scatter",
    )(blocks)


def shards(
    tokens,
    norm_gain,
    conv_value_weight,
    conv_gate_weight,
    conv_kernel,
    conv_bias,
    channel_gain,
    query_weight,
    key_weight,
    value_weight,
    gate_weight,
    gate_offset,
    start_memory,
    start_norm,
    start_level,
    cell_gain,
    out_conv_weight,
    out_cell_weight,
):
    parts = lax.axis_size(HEAD)
    groups = lax.axis_size(OUTER)
    group = lax.axis_index(OUTER)
    part = lax.axis_index(HEAD)
    key_width = start_norm.shape[2]
    value_width = start_memory.shape[2]
    all_channels = conv_bias.shape[0] * lax.axis_size(TP)
    heads_here = start_level.shape[1]
    channels = conv_bias.shape[0] // parts

    features = tokens.astype(jnp.float32)
    normed = (
        features * lax.rsqrt(jnp.mean(features * features, axis=1, keepdims=True) + EPS) * norm_gain
    ).astype(jnp.bfloat16)

    gate_pre = jnp.dot(normed, gate_weight, preferred_element_type=jnp.float32)
    gate_pre = gate_pre.reshape(gate_pre.shape[0], 2, 2, gate_weight.shape[1] // 4)
    gate_pre = lax.dynamic_slice_in_dim(gate_pre, lax.axis_index(TP) * heads_here, heads_here, 3)
    gate_pre = jnp.transpose(gate_pre, (1, 2, 3, 0)) + gate_offset
    direct = 1 < parts and groups * parts <= 16
    if direct:
        rows, gates, key_value_part, other_part, out_rows = exchange(
            groups,
            parts,
            normed,
            gate_pre,
            key_weight,
            value_weight,
            conv_value_weight,
            conv_gate_weight,
            query_weight,
            out_conv_weight,
            out_cell_weight,
        )
        gates = lax.dynamic_index_in_dim(gates, part, 3, False)
        gates = jnp.transpose(gates, (1, 2, 0, 3)).reshape(gates.shape[1:3] + (-1,))
    else:
        gates = lax.all_gather(gate_pre, (OUTER, HEAD), axis=3, tiled=True)
        gates = lax.dynamic_index_in_dim(gates, part, 2, False)
        rows = lax.all_gather(normed, HEAD, axis=0, tiled=True)
        key_value_part = lax.all_gather(
            spread(by_head((key_weight, value_weight), parts)), OUTER, axis=0, tiled=True
        )
        other_part = lax.all_gather(
            spread(by_head((conv_value_weight, conv_gate_weight, query_weight), parts)),
            OUTER,
            axis=0,
            tiled=True,
        )
        out_rows = spread(by_head((out_conv_weight, out_cell_weight), parts))
    here = rows.shape[0]
    out_part = lax.all_gather(out_rows, OUTER, axis=0, tiled=True)

    key_value = jnp.dot(rows, key_value_part, preferred_element_type=jnp.float32).astype(
        jnp.bfloat16
    )
    others = jnp.dot(rows, other_part, preferred_element_type=jnp.float32).astype(jnp.bfloat16)
    queries = others[:, 2 * channels :]

    gated = (
        others[:, :channels].astype(jnp.float32)
        * jax.nn.sigmoid(others[:, channels : 2 * channels].astype(jnp.float32))
    ).astype(jnp.bfloat16)
    reach = conv_kernel.shape[0] // 2
    up = [(i, i + 1) for i in range(groups - 1)]
    down = [(j, i) for i, j in up]
    before = lax.ppermute(gated[here - reach :], OUTER, up)
    after = lax.ppermute(gated[:reach], OUTER, down)
    key_value, before, after = lax.optimization_barrier((key_value, before, after))
    if direct:
        around = [key_value] + [
            lax.ppermute(key_value, OUTER, [(i, (i + g) % groups) for i in range(groups)])
            for g in range(1, groups)
        ]
        sources = [lax.rem(group + groups - g, groups) for g in range(groups)]
        all_key_value = jnp.concatenate(around, axis=0)
    else:
        all_key_value = lax.all_gather(key_value, OUTER, axis=0, tiled=True)
    padded = jnp.concatenate([before, gated, after], axis=0).astype(jnp.float32)
    taps = own_columns(conv_kernel, parts, part)
    conv_sum = own_columns(conv_bias, parts, part) + sum(
        taps[offset] * padded[offset : offset + here] for offset in range(conv_kernel.shape[0])
    )
    stats = lax.psum(
        jnp.stack([jnp.sum(conv_sum, axis=1), jnp.sum(conv_sum * conv_sum, axis=1)]), (HEAD, TP)
    )
    channel_mean = stats[0] / all_channels
    channel_var = stats[1] / all_channels - channel_mean * channel_mean
    conv_out = jax.nn.silu(
        (conv_sum - channel_mean[:, None])
        * lax.rsqrt(channel_var + EPS)[:, None]
        * own_columns(channel_gain, parts, part)
    ).astype(jnp.bfloat16)

    total = gates.shape[2]
    in_gate = gates[:, 0]
    log_forget = jax.nn.log_sigmoid(gates[:, 1])
    whole = jnp.round(log_forget)
    both = jnp.stack([whole, log_forget - whole])
    both = jnp.stack([both[:, 0], jnp.flip(both[:, 1], axis=1)], axis=1)
    both = running_sum(both)
    passed = jnp.stack([both[:, 0], jnp.flip(both[:, 1], axis=1)], axis=1)
    passed_here = lax.dynamic_slice_in_dim(passed, group * here, here, 2)
    at_column = jnp.arange(total)
    if direct:

        def around_ring(array):
            return jnp.concatenate(
                [lax.dynamic_slice_in_dim(array, g * here, here, array.ndim - 1) for g in sources],
                axis=-1,
            )

        at_column, in_gate, passed = (around_ring(a) for a in (at_column, in_gate, passed))
    at_column = at_column[None, :]
    keys = all_key_value[:, :key_width]
    values = all_key_value[:, key_width:]
    products = lax.dot_general(
        queries, keys, (((1,), (1,)), ((), ())), preferred_element_type=jnp.float32
    ) * (key_width**-0.5)
    at_row = (group * here + jnp.arange(here))[:, None]
    levels = lax.dynamic_index_in_dim(start_level, part, 1, False)
    norms = lax.dynamic_index_in_dim(start_norm, part, 1, False)
    memories = lax.dynamic_index_in_dim(start_memory, part, 1, False)
    wide_queries = queries.astype(jnp.float32)
    scaled = 0.0
    entered = 0.0
    for way in range(2):
        row_whole, row_rest = passed_here[0, way], passed_here[1, way]
        table = (row_whole[:, None] - passed[0, way][None, :]) + (
            row_rest[:, None] + (in_gate[way] - passed[1, way])[None, :]
        )
        seen = at_column <= at_row if way == 0 else at_column >= at_row
        table = jnp.where(seen, table, -jnp.inf)
        start = row_whole + row_rest + levels[way]
        top = jnp.maximum(start, jnp.max(table, axis=1))
        scores = products * jnp.exp(table - top[:, None])
        entry = jnp.exp(start - top)
        denominator = jnp.sum(scores, axis=1) + entry * jnp.sum(
            wide_queries * norms[way][None, :], axis=1
        )
        inverse = 1.0 / jnp.maximum(jnp.abs(denominator), 1.0)
        scaled = scaled + scores * inverse[:, None]
        entered = entered + (entry * inverse)[:, None] * lax.dot_general(
            queries,
            memories[way].astype(jnp.bfloat16),
            (((1,), (1,)), ((), ())),
            preferred_element_type=jnp.float32,
        )
    both_ways = entered + jnp.dot(
        scaled.astype(jnp.bfloat16), values, preferred_element_type=jnp.float32
    )
    both_ways = both_ways * lax.rsqrt(jnp.mean(both_ways * both_ways, axis=1, keepdims=True) + EPS)
    cell_out = (both_ways * own_columns(cell_gain, parts, part)).astype(jnp.bfloat16)

    partial = lax.dot_general(
        jnp.concatenate([conv_out, cell_out], axis=1),
        out_part,
        (((1,), (1,)), ((), ())),
        preferred_element_type=jnp.float32,
    ).astype(jnp.bfloat16)
    if direct and lax.axis_size(TP) == 2:
        return scatter(parts, partial)
    return lax.psum_scatter(partial, (HEAD, TP), scatter_dimension=0, tiled=True)


AXES = ("z", "y", "x", "tp")


def tile_at(index, size):
    return pl.ds(pl.multiple_of(index * size, size), size)


class Copies:
    def __init__(self, send, recv):
        self.send, self.recv, self.count = send, recv, 0

    def take(self, many=1):
        first = self.count
        self.count += many
        return first

    def remote(self, index, source, target, device):
        return pltpu.make_async_remote_copy(
            src_ref=source,
            dst_ref=target,
            send_sem=self.send.at[index],
            recv_sem=self.recv.at[index],
            device_id=device,
            device_id_type=MESH,
        )


def when(condition, action):
    if condition is True:
        action()
    else:
        pl.when(condition)(action)


def gather_kernel(
    tokens, gain, gate_weight, gate_offset, query, key, value, conv_value, conv_gate,
    projected, gates, rows, weights, turned, picked, send, recv, local,
):
    z, y, x, tp = (lax.axis_index(axis) for axis in AXES)
    planes, lines, columns = lax.axis_size("z"), lax.axis_size("y"), lax.axis_size("x")
    depth, model = tokens.shape
    key_width = query.shape[1] // planes
    value_width = value.shape[1] // planes // columns
    conv_width = conv_value.shape[1] // planes
    half = depth // 2
    pool = Copies(send, recv)

    barrier = pltpu.get_barrier_semaphore()
    steps = [
        (a, b, c)
        for a in range(planes)
        for b in range(lines)
        for c in range(columns)
        if (a, b, c) != (0, 0, 0)
    ]

    def device(step):
        return {
            "z": lax.rem(z + step[0], planes),
            "y": lax.rem(y + step[1], lines),
            "x": lax.rem(x + step[2], columns),
        }

    for step in steps:
        pl.semaphore_signal(barrier, inc=1, device_id=device(step), device_id_type=MESH)
    pl.semaphore_signal(barrier, inc=1, device_id={"tp": 1 - tp}, device_id_type=MESH)
    pl.semaphore_wait(barrier, len(steps) + 1)

    def place(a, b, c):
        return (a * lines + b) * columns + c

    def piece(a, c):
        return tile_at(place(a, y, c), depth)

    mine = piece(z, x)

    def sources(a, c):
        wide = pl.ds(pl.multiple_of((a * columns + c) * value_width, 128), value_width)
        narrow, gated = tile_at(a, key_width), tile_at(a, conv_width)
        first = pl.ds(0, key_width)
        second = pl.ds(key_width, value_width)
        third = pl.ds(key_width + value_width, conv_width)
        return [
            (c == 0, query.at[:, narrow], weights.at[mine, first], 0),
            (c == 1, key.at[:, narrow], weights.at[mine, first], 0),
            (True, value.at[:, wide], weights.at[mine, second], 1),
            (c == 0, conv_value.at[:, gated], weights.at[mine, third], 2),
            (c == 1, conv_gate.at[:, gated], weights.at[mine, third], 2),
        ]

    direct = pool.take(3 * planes * columns)

    def weight_copies(a, c):
        found = []
        to_z, to_x = lax.rem(z + a, planes), lax.rem(x + c, columns)
        for condition, source, target, kind in sources(to_z, to_x):
            index = direct + 3 * (a * columns + c) + kind
            found.append((condition, pool.remote(index, source, target, {"z": to_z, "x": to_x})))
        return found

    def send_weights(a, c):
        for condition, copy in weight_copies(a, c):
            when(condition, copy.start)

    kept = [
        (condition, pltpu.make_async_copy(source, target, local.at[kind]))
        for condition, source, target, kind in sources(z, x)
    ]
    for condition, copy in kept:
        when(condition, copy.start)
    send_weights(0, 1)
    send_weights(2, 0)

    small = 16

    def normalize(step, carry):
        at = tile_at(step, small)
        features = tokens[at].astype(jnp.float32)
        scale = lax.rsqrt(jnp.mean(features * features, axis=1, keepdims=True) + EPS)
        base = pl.multiple_of((z * columns + x) * depth + step * small, small)
        rows[pl.ds(base, small)] = (features * scale * gain[...]).astype(rows.dtype)
        return carry

    lax.fori_loop(0, depth // small, normalize, 0)

    def block(a, c, part):
        return rows.at[tile_at((a * columns + c) * 2 + part, half)]

    up, down = pool.take(planes), pool.take(planes)
    across, over = pool.take(2 * planes), pool.take(4 * planes)

    def chain(first, sign, step):
        held = z - sign * (step - 1)
        able = (held >= 0) & (held < planes) & (z + sign >= 0) & (z + sign < planes)
        part = block(held, x, tp)
        return able, pool.remote(first + step, part, part, {"z": z + sign})

    def arrived(sign, step):
        return (z - sign * step >= 0) & (z - sign * step < planes)

    def to_x(slot, a):
        part = block(a, x, tp)
        return pool.remote(across + slot, part, part, {"x": 1 - x})

    def to_core(slot, a, c):
        part = block(a, c, tp)
        return pool.remote(over + slot, part, part, {"tp": 1 - tp})

    for first, sign in ((up, 1), (down, -1)):
        able, copy = chain(first, sign, 1)
        when(able, copy.start)
    to_x(0, z).start()
    send_weights(1, 0)
    send_weights(3, 0)

    plain = jnp.dot(
        rows[tile_at(z * columns + x, depth)], gate_weight[...], preferred_element_type=jnp.float32
    )
    turned[: plain.shape[1]] = jnp.transpose(plain)
    heads = plain.shape[1] // 4
    for way in range(2):
        for kind in range(2):
            for head in range(planes):
                at = (way * 2 + kind) * heads + tp * planes + head
                picked[head, way * 2 + kind : way * 2 + kind + 1] = (
                    turned[pl.ds(at, 1)] + gate_offset[way, kind, head : head + 1]
                )
    own = place(z, y, x)
    gates[own] = picked[z]
    spread_gates = pool.take(len(steps))
    gate_copies = [
        pool.remote(
            spread_gates + number,
            picked.at[lax.rem(z + step[0], planes)],
            gates.at[own],
            device(step),
        )
        for number, step in enumerate(steps)
    ]
    for copy in gate_copies:
        copy.start()

    relay = pool.take(planes * columns)

    def relay_copy(a, c):
        from_z, from_x = lax.rem(z + planes - a, planes), lax.rem(x + columns - c, columns)
        part = weights.at[piece(from_z, from_x)]
        return pool.remote(relay + a * columns + c, part, part, {"y": 1 - y})

    for condition, copy in kept:
        when(condition, copy.wait)
    relay_copy(0, 0).start()

    def take_weights(a, c):
        for condition, copy in weight_copies(a, c):
            when(condition, copy.wait_recv)
        relay_copy(a, c).start()

    def take_tokens(step):
        for number, (first, sign) in enumerate(((up, 1), (down, -1))):
            held = z - sign * step

            def forward(first=first, sign=sign, number=number, held=held):
                chain(first, sign, step)[1].wait_recv()
                if step + 1 < planes:
                    able, copy = chain(first, sign, step + 1)
                    when(able, copy.start)
                slot = number * planes + step
                to_x(slot, held).start()
                to_core(slot, held, x).start()

            when(arrived(sign, step), forward)

    def cross_tokens(step):
        if step == 0:
            to_x(0, z).wait_recv()
            to_core(2 * planes, z, 1 - x).start()
            return
        for number, sign in enumerate((1, -1)):
            held = z - sign * step
            slot = number * planes + step

            def forward(slot=slot, held=held):
                to_x(slot, held).wait_recv()
                to_core(2 * planes + slot, held, 1 - x).start()

            when(arrived(sign, step), forward)

    take_weights(0, 1)
    cross_tokens(0)
    take_tokens(1)
    send_weights(1, 1)
    send_weights(3, 1)
    take_weights(1, 0)
    take_weights(3, 0)
    take_tokens(2)
    send_weights(2, 1)
    take_weights(2, 0)
    cross_tokens(1)
    take_tokens(3)
    take_weights(1, 1)
    take_weights(3, 1)
    cross_tokens(2)
    take_weights(2, 1)
    cross_tokens(3)

    def tokens_over():
        found = []
        for number, sign in enumerate((1, -1)):
            for step in range(1, planes):
                held = z - sign * step
                slot = number * planes + step
                for copy in (to_core(slot, held, x), to_core(2 * planes + slot, held, 1 - x)):
                    found.append((arrived(sign, step), copy))
        found.append((True, to_core(2 * planes, z, 1 - x)))
        return found

    for condition, copy in tokens_over():
        when(condition, copy.wait_recv)
    for a in range(planes):
        for c in range(columns):
            relay_copy(a, c).wait_recv()

    tall = 2 * depth

    def project(step, carry):
        at = tile_at(step, tall)
        projected[at] = jnp.dot(
            rows[at], weights[...], preferred_element_type=jnp.float32
        ).astype(projected.dtype)
        return carry

    lax.fori_loop(0, rows.shape[0] // tall, project, 0)

    for copy in gate_copies:
        copy.wait()
    for a in range(planes):
        for c in range(columns):
            relay_copy(a, c).wait_send()
            if (a, c) != (0, 0):
                for condition, copy in weight_copies(a, c):
                    when(condition, copy.wait_send)
    for first, sign in ((up, 1), (down, -1)):
        for step in range(1, planes):
            able, copy = chain(first, sign, step)
            when(able, copy.wait_send)
    to_x(0, z).wait_send()
    for number, sign in enumerate((1, -1)):
        for step in range(1, planes):
            when(arrived(sign, step), to_x(number * planes + step, z - sign * step).wait_send)
    for condition, copy in tokens_over():
        when(condition, copy.wait_send)


VMEM_SPEC = pl.BlockSpec(memory_space=pltpu.VMEM)
ANY_SPEC = pl.BlockSpec(memory_space=pl.ANY)


def gather(tokens, gain, gate_weight, gate_offset, query, key, value, conv_value, conv_gate):
    planes, lines, columns = (lax.axis_size(a) for a in AXES[:3])
    depth, model = tokens.shape
    wide = (query.shape[1] + value.shape[1] // columns + conv_value.shape[1]) // planes
    tall = planes * columns * depth
    blocks = planes * lines * columns
    many = 4 * planes * columns + 2 * planes + 6 * planes + blocks - 1
    f32, bf16 = jnp.float32, jnp.bfloat16
    return pl.pallas_call(
        gather_kernel,
        out_shape=(
            jax.ShapeDtypeStruct((tall, wide), bf16),
            jax.ShapeDtypeStruct((blocks, 4, depth), f32),
        ),
        in_specs=[VMEM_SPEC] * 4 + [ANY_SPEC] * 5,
        out_specs=(VMEM_SPEC, VMEM_SPEC),
        scratch_shapes=[
            pltpu.VMEM((tall, model), bf16),
            pltpu.VMEM((model, wide), bf16),
            pltpu.VMEM((depth, depth), f32),
            pltpu.VMEM((planes, 4, depth), f32),
            pltpu.SemaphoreType.DMA((many,)),
            pltpu.SemaphoreType.DMA((many,)),
            pltpu.SemaphoreType.DMA((3,)),
        ],
        compiler_params=pltpu.CompilerParams(collective_id=3, has_side_effects=True),
        name="gather",
    )(tokens, gain, gate_weight, gate_offset, query, key, value, conv_value, conv_gate)


def prefix(values, way):
    count, length = values.shape
    lane = lax.broadcasted_iota(jnp.int32, values.shape, 1)
    row = lax.broadcasted_iota(jnp.int32, values.shape, 0)
    shift = 1
    while shift < length:
        if way == 0:
            values = values + jnp.where(lane >= shift, pltpu.roll(values, shift, 1), 0.0)
        else:
            moved = pltpu.roll(values, length - shift, 1)
            values = values + jnp.where(lane < length - shift, moved, 0.0)
        shift *= 2
    last = values[:, length - 1 :] if way == 0 else values[:, :1]
    totals = jnp.broadcast_to(last, values.shape)
    before = totals
    shift = 1
    while shift < count:
        if way == 0:
            before = before + jnp.where(row >= shift, pltpu.roll(before, shift, 0), 0.0)
        else:
            moved = pltpu.roll(before, count - shift, 0)
            before = before + jnp.where(row < count - shift, moved, 0.0)
        shift *= 2
    return values + (before - totals)


NT = (((1,), (1,)), ((), ()))


def cell_kernel(
    projected, gates, taps, bias, channel_gain, start_norm, cell_gain, start_level, start_memory,
    out_conv, out_cell,
    out,
    pair, far_key, far_value, conv_half, gated, edge, padded, conv_sum, stats, conv_out,
    total, row_form, flat, columns_of, top, weight_sum, acc, memory, both, squares,
    features, conv_weights, cell_weights, part, near, near_sum, cross, cross_sum, cross_send,
    landed, send, recv, local,
):
    z, y, x, tp = (lax.axis_index(axis) for axis in AXES)
    planes, lines, columns = lax.axis_size("z"), lax.axis_size("y"), lax.axis_size("x")
    blocks, _, depth = gates.shape
    key_width = pair.shape[2]
    value_width = far_value.shape[1]
    conv_width = conv_half.shape[1]
    tall = 2 * depth
    chunks = planes
    f32, bf16 = jnp.float32, jnp.bfloat16
    scale = key_width**-0.5
    halo = edge.shape[2]
    pool = Copies(send, recv)

    barrier = pltpu.get_barrier_semaphore()
    peers = []
    for a in range(planes):
        for c in range(columns):
            for core in range(2):
                if (a, c, core) != (0, 0, 0) and not (c == 1 and core == 1):
                    peers.append(
                        {
                            "z": lax.rem(z + a, planes),
                            "x": lax.rem(x + c, columns),
                            "tp": lax.rem(tp + core, 2),
                        }
                    )
    peers.append({"y": 1 - y})
    for peer in peers:
        pl.semaphore_signal(barrier, inc=1, device_id=peer, device_id_type=MESH)
    pl.semaphore_wait(barrier, len(peers))

    def chunk(c):
        return tile_at(c, tall)

    keys = pl.ds(0, key_width)
    values = pl.ds(key_width, value_width)
    convs = pl.ds(key_width + value_width, conv_width)

    side = pool.take()
    side_copy = pool.remote(side, projected.at[:, convs], conv_half, {"x": 1 - x})
    side_copy.start()
    pair_at = pool.take(chunks)
    pair_copies = [
        pool.remote(
            pair_at + c, projected.at[chunk(c), keys], pair.at[x, chunk(c)], {"x": 1 - x}
        )
        for c in range(chunks)
    ]
    for copy in pair_copies:
        copy.start()
    value_at = pool.take(chunks)
    value_copies = [
        pool.remote(
            value_at + c, projected.at[chunk(c), values], far_value.at[chunk(c)], {"y": 1 - y}
        )
        for c in range(chunks)
    ]
    for copy in value_copies:
        copy.start()
    memory_copies = [
        pltpu.make_async_copy(
            start_memory.at[way, z, tile_at(x, value_width)], memory.at[way], local.at[way]
        )
        for way in range(2)
    ]
    for copy in memory_copies:
        copy.start()

    model_block = out_conv.shape[0]

    def place(a, b, c):
        return (a * lines + b) * columns + c

    mine = tile_at(place(z, y, x), model_block)

    def out_sources(a, c):
        wide = pl.ds(pl.multiple_of((a * columns + c) * value_width, 128), value_width)
        return (
            (out_conv.at[:, tile_at(a, conv_width)], conv_weights.at[mine]),
            (out_cell.at[:, wide], cell_weights.at[mine]),
        )

    out_at = pool.take(2 * planes * columns)

    def out_copies(a, c):
        to_z, to_x = lax.rem(z + a, planes), lax.rem(x + c, columns)
        return [
            pool.remote(
                out_at + 2 * (a * columns + c) + kind, source, target, {"z": to_z, "x": to_x}
            )
            for kind, (source, target) in enumerate(out_sources(to_z, to_x))
        ]

    others = [(a, c) for a in range(planes) for c in range(columns) if (a, c) != (0, 0)]
    for a, c in others:
        for copy in out_copies(a, c):
            copy.start()
    out_kept = [
        pltpu.make_async_copy(source, target, local.at[2 + kind])
        for kind, (source, target) in enumerate(out_sources(z, x))
    ]
    for copy in out_kept:
        copy.start()

    pair[x] = projected[:, :key_width]

    for way in range(2):
        in_gate = gates[:, 2 * way, :]
        forget = gates[:, 2 * way + 1, :]
        log_forget = jnp.minimum(forget, 0.0) - jnp.log1p(jnp.exp(-jnp.abs(forget)))
        whole = jnp.round(log_forget)
        passed = prefix(whole, way)
        rest = prefix(log_forget - whole, way)
        total[2 * way] = passed
        total[2 * way + 1] = rest
        against = in_gate - rest
        for g in range(blocks // 2):
            for h in range(2):
                at = slice(2 * g + h, 2 * g + h + 1)
                row_form[2 * way, h, g : g + 1] = passed[at]
                row_form[2 * way + 1, h, g : g + 1] = against[at]
    flat[...] = jnp.zeros_like(flat)
    for q in range(4):
        for c in range(chunks):
            flat[q * 8 + 2 * c : q * 8 + 2 * c + 2] = total[
                q, pl.ds(c * lines * columns + y * columns, 2)
            ]
    turned = jnp.transpose(flat[...])
    for q in range(4):
        for b in range(2 * chunks):
            columns_of[q, b * depth : (b + 1) * depth] = jnp.broadcast_to(
                turned[:, q * 8 + b : q * 8 + b + 1], (depth, depth)
            )

    def column_mask(h, way):
        row = lax.broadcasted_iota(jnp.int32, (tall, depth), 0)
        lane = lax.broadcasted_iota(jnp.int32, (tall, depth), 1) + h * depth
        return lane <= row if way == 0 else lane >= row

    def row_of(q, h, g):
        return row_form[q, h, pl.ds(g, 1)]

    def find_top(c, carry):
        rows = chunk(c)
        here = lines * c + y

        for way in range(2):
            best = None
            for h in range(2):
                table = (columns_of[2 * way, rows] - row_of(2 * way, h, here)) + (
                    columns_of[2 * way + 1, rows] + row_of(2 * way + 1, h, here)
                )
                table = jnp.where(column_mask(h, way), table, -jnp.inf)
                best = table if best is None else jnp.maximum(best, table)
            top[way, rows] = best

        def step(g, inner):
            way = jnp.where(g < here, 0, 1)

            @pl.when(g != here)
            def _():
                best = top[way, rows]
                for h in range(2):
                    table = (columns_of[2 * way, rows] - row_of(2 * way, h, g)) + (
                        columns_of[2 * way + 1, rows] + row_of(2 * way + 1, h, g)
                    )
                    best = jnp.maximum(best, table)
                top[way, rows] = best

            return inner

        lax.fori_loop(0, lines * chunks, step, 0)
        for way in range(2):
            start = columns_of[2 * way, rows] + columns_of[2 * way + 1, rows] + start_level[way, z]
            best = jnp.max(top[way, rows], axis=1, keepdims=True)
            top[way, rows] = jnp.maximum(start, jnp.broadcast_to(best, (tall, depth)))
            columns_of[2 * way + 1, rows] = columns_of[2 * way + 1, rows] - top[way, rows]
        return carry

    lax.fori_loop(0, chunks, find_top, 0)

    edge_at = pool.take()
    edge_copy = pool.remote(edge_at, edge.at[0], edge.at[1], {"y": 1 - y})
    side_copy.wait_recv()

    def gate_rows(c, carry):
        rows = chunk(c)
        mine_half = projected[rows, key_width + value_width :].astype(f32)
        their_half = conv_half[rows].astype(f32)
        value_side = jnp.where(x == 0, mine_half, their_half)
        gate_side = jnp.where(x == 0, their_half, mine_half)
        gated[rows] = (value_side * jax.nn.sigmoid(gate_side)).astype(bf16)
        return carry

    lax.fori_loop(0, chunks, gate_rows, 0)
    for c in range(chunks):
        base = c * tall + jnp.where(x == 0, tall - halo, 0)
        edge[0, c] = gated[pl.ds(pl.multiple_of(base, halo), halo)]
    edge_copy.start()

    key_at = pool.take(chunks)
    key_copies = [
        pool.remote(key_at + c, pair.at[1, chunk(c)], far_key.at[chunk(c)], {"y": 1 - y})
        for c in range(chunks)
    ]
    for c in range(chunks):
        pair_copies[c].wait_recv()
        key_copies[c].start()

    out_relay = pool.take(2 * planes * columns)

    def out_relays(a, c):
        from_z, from_x = lax.rem(z + planes - a, planes), lax.rem(x + columns - c, columns)
        at = tile_at(place(from_z, y, from_x), model_block)
        return [
            pool.remote(
                out_relay + 2 * (a * columns + c) + kind, ref.at[at], ref.at[at], {"y": 1 - y}
            )
            for kind, ref in enumerate((conv_weights, cell_weights))
        ]

    for copy in out_kept:
        copy.wait()
    for copy in out_relays(0, 0):
        copy.start()

    edge_copy.wait_recv()
    channel = tile_at(z, conv_width)
    flat[...] = jnp.zeros_like(flat)
    lane = lax.broadcasted_iota(jnp.int32, (depth, depth), 1)
    table = jnp.zeros((depth, depth), f32)
    for c in range(chunks):
        mine_rows = gated[pl.ds(pl.multiple_of(c * tall + x * depth, depth), depth)]
        padded[pl.ds(halo, depth)] = mine_rows.astype(f32)
        low_at = c - (1 - y)
        low = edge[1, jnp.maximum(low_at, 0)].astype(f32)
        low = jnp.where(low_at >= 0, low, 0.0)
        low = jnp.where(x == 0, low, gated[c * tall + depth - halo : c * tall + depth].astype(f32))
        high_at = c + y
        high = edge[1, jnp.minimum(high_at, chunks - 1)].astype(f32)
        high = jnp.where(high_at < chunks, high, 0.0)
        high = jnp.where(
            x == 0, gated[c * tall + depth : c * tall + depth + halo].astype(f32), high
        )
        padded[pl.ds(0, halo)] = low
        padded[pl.ds(halo + depth, halo)] = high
        reach = taps.shape[0] // 2
        value = jnp.broadcast_to(bias[:, channel], (depth, conv_width))
        for tap in range(taps.shape[0]):
            value = value + taps[tap : tap + 1, channel] * padded[
                pl.ds(halo - reach + tap, depth)
            ]
        conv_sum[c] = value
        plain = jnp.sum(value, axis=1, keepdims=True)
        square = jnp.sum(value * value, axis=1, keepdims=True)
        table = jnp.where(lane == c, plain, table)
        table = jnp.where(lane == chunks + c, square, table)
    stats[0] = jnp.transpose(table)[: 2 * chunks]
    stat_at = pool.take(2 * planes)
    stat_copies = []
    for a in range(planes):
        for core in range(2):
            if (a, core) != (0, 0):
                number = a * 2 + core
                stat_copies.append(
                    pool.remote(
                        stat_at + number,
                        stats.at[0],
                        stats.at[number],
                        {"z": lax.rem(z + a, planes), "tp": lax.rem(tp + core, 2)},
                    )
                )
                stat_copies[-1].start()

    def tile(c, g, keys_ref, values_ref, way, mask):
        rows = chunk(c)
        products = lax.dot_general(pair[0, rows], keys_ref, NT, preferred_element_type=f32)
        pieces = []
        for h in range(2):
            level = (columns_of[2 * way, rows] - row_of(2 * way, h, g)) + (
                columns_of[2 * way + 1, rows] + row_of(2 * way + 1, h, g)
            )
            if mask:
                level = jnp.where(column_mask(h, way), level, -jnp.inf)
            pieces.append(products[:, h * depth : (h + 1) * depth] * jnp.exp(level))
        scores = jnp.concatenate(pieces, axis=1).astype(bf16)
        summed = pieces[0] + pieces[1]
        added = jnp.dot(scores, values_ref, preferred_element_type=f32)
        if mask:
            weight_sum[way, rows] = summed
            acc[way, rows] = added
        else:
            weight_sum[way, rows] += summed
            acc[way, rows] += added

    def diagonal(c, carry):
        for way in range(2):
            tile(
                c, lines * c + y, pair[1, chunk(c)],
                projected[chunk(c), key_width : key_width + value_width], way, True,
            )
        return carry

    lax.fori_loop(0, chunks, diagonal, 0)

    def own_step(number, carry):
        c, s = number // chunks, lax.rem(number, chunks)

        @pl.when(c != s)
        def _():
            tile(
                c, lines * s + y, pair[1, chunk(s)],
                projected[chunk(s), key_width : key_width + value_width],
                jnp.where(s < c, 0, 1), False,
            )

        return carry

    lax.fori_loop(0, chunks * chunks, own_step, 0)

    for a, c in others:
        for copy in out_copies(a, c):
            copy.wait_recv()
        for copy in out_relays(a, c):
            copy.start()

    for copy in stat_copies:
        copy.wait_recv()
    stat_sum = stats[0]
    for number in range(1, 2 * planes):
        stat_sum = stat_sum + stats[number]
    flat[: 2 * chunks] = stat_sum / (conv_width * planes * 2)
    turned = jnp.transpose(flat[...])
    for c in range(chunks):
        mean = turned[:, c : c + 1]
        var = turned[:, chunks + c : chunks + c + 1] - mean * mean
        conv_out[c * depth : (c + 1) * depth] = jax.nn.silu(
            (conv_sum[c] - mean) * lax.rsqrt(var + EPS) * channel_gain[:, channel]
        ).astype(bf16)

    for s in range(chunks):
        value_copies[s].wait_recv()
        key_copies[s].wait_recv()

        def far_step(c, carry, s=s):
            g = lines * s + (1 - y)
            way = jnp.where(g < lines * c + y, 0, 1)
            tile(c, g, far_key[chunk(s)], far_value[chunk(s)], way, False)
            return carry

        lax.fori_loop(0, chunks, far_step, 0)

    for copy in memory_copies:
        copy.wait()
    squares[0] = jnp.zeros_like(squares[0])

    def finish(c, table):
        rows = chunk(c)
        query = pair[0, rows]
        result = jnp.zeros((tall, value_width), f32)
        for way in range(2):
            entered = lax.dot_general(
                query, memory[way].astype(bf16), NT, preferred_element_type=f32
            )
            entry = jnp.exp(
                columns_of[2 * way, rows] + (columns_of[2 * way + 1, rows] + start_level[way, z])
            )[:, :1]
            normed = jnp.sum(
                query.astype(f32) * start_norm[way, pl.ds(z, 1)], axis=1, keepdims=True
            )
            below = scale * jnp.sum(weight_sum[way, rows], axis=1, keepdims=True) + entry * normed
            inverse = 1.0 / jnp.maximum(jnp.abs(below), 1.0)
            result = result + (scale * acc[way, rows] + entry * entered) * inverse
        both[rows] = result
        square = jnp.sum(result * result, axis=1, keepdims=True)
        for h in range(2):
            table = jnp.where(lane == 2 * c + h, square[h * depth : (h + 1) * depth], table)
        return table

    table = lax.fori_loop(0, chunks, finish, jnp.zeros((depth, depth), f32))
    square_at = pool.take()
    squares[0] = jnp.transpose(table)[: 2 * chunks]
    square_copy = pool.remote(square_at, squares.at[0], squares.at[1], {"x": 1 - x})
    square_copy.start()
    square_copy.wait_recv()
    flat[: 2 * chunks] = (squares[0] + squares[1]) / (value_width * columns)
    turned = jnp.transpose(flat[...])
    gain = cell_gain[:, pl.ds(pl.multiple_of((z * columns + x) * value_width, 128), value_width)]
    for b in range(2 * chunks):
        at = slice(b * depth, (b + 1) * depth)
        features[at] = (both[at] * lax.rsqrt(turned[:, b : b + 1] + EPS) * gain).astype(bf16)

    half = depth // 2
    wide = part.shape[-1]
    near_at, cross_at = pool.take(2 * chunks), pool.take(2 * chunks)
    land_at = pool.take(2 * chunks * planes)

    def near_copy(n):
        return pool.remote(near_at + n, part.at[n, 1 - tp], near.at[n], {"tp": 1 - tp})

    def cross_copy(n):
        return pool.remote(cross_at + n, near_sum.at[n], cross.at[n], {"x": 1 - x})

    def land_copy(n, a):
        return pool.remote(
            land_at + n * planes + a,
            cross_send.at[n, lax.rem(z + a, planes)],
            landed.at[n, a],
            {"z": lax.rem(z + a, planes)},
        )

    def model_rows(n):
        line = y if n < chunks else 1 - y
        return lax.rem(n, chunks) * lines + line

    def multiply(n):
        at = chunk(model_rows(n))

        def step(a, carry):
            rows = chunk(a)
            found = lax.dot_general(
                features[rows], cell_weights[at], NT, preferred_element_type=f32
            )
            from_conv = lax.dot_general(
                conv_out[tile_at(a, depth)], conv_weights[at], NT, preferred_element_type=f32
            )
            for c in range(columns):
                mine_part = found[c * depth : (c + 1) * depth]
                mine_part = mine_part + jnp.where(x == c, from_conv, 0.0)
                for core in range(2):
                    part[n, core, c, a] = mine_part[core * half : (core + 1) * half].astype(bf16)
            return carry

        lax.fori_loop(0, planes, step, 0)

    def stage_near(n):
        near_copy(n).wait_recv()
        near_sum[n] = (
            part[n, tp, 1 - x].astype(f32) + near[n, 1 - x].astype(f32)
        ).astype(bf16)
        cross_copy(n).start()

    def stage_cross(n):
        cross_copy(n).wait_recv()
        summed = (
            part[n, tp, x].astype(f32) + near[n, x].astype(f32) + cross[n].astype(f32)
        )
        cross_sum[n] = summed
        cross_send[n] = summed.astype(bf16)
        for a in range(1, planes):
            land_copy(n, a).start()

    def stage_land(n):
        for a in range(1, planes):
            land_copy(n, a).wait_recv()
        summed = cross_sum[n, z]
        for a in range(1, planes):
            summed = summed + landed[n, a].astype(f32)
        out[:, chunk(model_rows(n))] = summed.astype(out.dtype)

    many = 2 * chunks
    for n in range(many + 3):
        if n < many:
            if n == chunks:
                for a in range(planes):
                    for c in range(columns):
                        for copy in out_relays(a, c):
                            copy.wait_recv()
            multiply(n)
            near_copy(n).start()
        if 0 <= n - 1 < many:
            stage_near(n - 1)
        if 0 <= n - 2 < many:
            stage_cross(n - 2)
        if 0 <= n - 3 < many:
            stage_land(n - 3)

    side_copy.wait_send()
    edge_copy.wait_send()
    square_copy.wait_send()
    for copy in pair_copies + value_copies + key_copies + stat_copies:
        copy.wait_send()
    for a, c in others:
        for copy in out_copies(a, c):
            copy.wait_send()
    for a in range(planes):
        for c in range(columns):
            for copy in out_relays(a, c):
                copy.wait_send()
    for n in range(many):
        near_copy(n).wait_send()
        cross_copy(n).wait_send()
        for a in range(1, planes):
            land_copy(n, a).wait_send()


def cell(
    projected, gates, taps, bias, channel_gain, start_norm, cell_gain, start_level, start_memory,
    out_conv, out_cell,
):
    planes, lines, columns = (lax.axis_size(a) for a in AXES[:3])
    blocks, _, depth = gates.shape
    key_width = start_norm.shape[2]
    value_width = start_memory.shape[2] // columns
    conv_width = bias.shape[1] // planes
    model_block = out_conv.shape[0]
    model = model_block * blocks
    tall = projected.shape[0]
    chunk = 2 * depth
    half = depth // 2
    pieces = model // chunk
    halo = 16
    f32, bf16 = jnp.float32, jnp.bfloat16
    many = 3 + 3 * planes + 4 * planes * columns + 2 * planes + 2 * pieces + pieces * planes
    return pl.pallas_call(
        cell_kernel,
        out_shape=jax.ShapeDtypeStruct((half, model), bf16),
        in_specs=[VMEM_SPEC] * 7
        + [pl.BlockSpec(memory_space=pltpu.SMEM)]
        + [ANY_SPEC] * 3,
        out_specs=VMEM_SPEC,
        scratch_shapes=[
            pltpu.VMEM((2, tall, key_width), bf16),
            pltpu.VMEM((tall, key_width), bf16),
            pltpu.VMEM((tall, value_width), bf16),
            pltpu.VMEM((tall, conv_width), bf16),
            pltpu.VMEM((tall, conv_width), bf16),
            pltpu.VMEM((2, planes, halo, conv_width), bf16),
            pltpu.VMEM((depth + 2 * halo, conv_width), f32),
            pltpu.VMEM((planes, depth, conv_width), f32),
            pltpu.VMEM((2 * planes, 2 * planes, depth), f32),
            pltpu.VMEM((planes * depth, conv_width), bf16),
            pltpu.VMEM((4, blocks, depth), f32),
            pltpu.VMEM((4, 2, blocks // 2, depth), f32),
            pltpu.VMEM((depth, depth), f32),
            pltpu.VMEM((4, tall, depth), f32),
            pltpu.VMEM((2, tall, depth), f32),
            pltpu.VMEM((2, tall, depth), f32),
            pltpu.VMEM((2, tall, value_width), f32),
            pltpu.VMEM((2, value_width, key_width), f32),
            pltpu.VMEM((tall, value_width), f32),
            pltpu.VMEM((2, 2 * planes, depth), f32),
            pltpu.VMEM((tall, value_width), bf16),
            pltpu.VMEM((model, conv_width), bf16),
            pltpu.VMEM((model, value_width), bf16),
            pltpu.VMEM((pieces, 2, columns, planes, half, chunk), bf16),
            pltpu.VMEM((pieces, columns, planes, half, chunk), bf16),
            pltpu.VMEM((pieces, planes, half, chunk), bf16),
            pltpu.VMEM((pieces, planes, half, chunk), bf16),
            pltpu.VMEM((pieces, planes, half, chunk), f32),
            pltpu.VMEM((pieces, planes, half, chunk), bf16),
            pltpu.VMEM((pieces, planes, half, chunk), bf16),
            pltpu.SemaphoreType.DMA((many,)),
            pltpu.SemaphoreType.DMA((many,)),
            pltpu.SemaphoreType.DMA((4,)),
        ],
        compiler_params=pltpu.CompilerParams(collective_id=4, has_side_effects=True),
        name="cell",
    )(
        projected, gates, taps, bias, channel_gain, start_norm, cell_gain, start_level,
        start_memory, out_conv, out_cell,
    )


def near_shards(
    tokens,
    norm_gain,
    conv_value_weight,
    conv_gate_weight,
    conv_kernel,
    conv_bias,
    channel_gain,
    query_weight,
    key_weight,
    value_weight,
    gate_weight,
    gate_offset,
    start_memory,
    start_norm,
    start_level,
    cell_gain,
    out_conv_weight,
    out_cell_weight,
):
    projected, gates = gather(
        tokens, norm_gain[None], gate_weight, gate_offset, query_weight, key_weight,
        value_weight, conv_value_weight, conv_gate_weight,
    )
    return cell(
        projected, gates, conv_kernel, conv_bias[None], channel_gain[None], start_norm,
        cell_gain[None], start_level, start_memory, out_conv_weight, out_cell_weight,
    )


def specs(split, TP):
    return (
        P(split, None),
        P(),
        P(split, TP),
        P(split, TP),
        P(None, TP),
        P(TP),
        P(TP),
        P(split, TP),
        P(split, TP),
        P(split, TP),
        P(),
        P(None, None, TP, split),
        P(None, TP, None, None),
        P(None, TP, None),
        P(None, TP),
        P(TP),
        P(split, TP),
        P(split, TP),
    )


def solution(mesh):
    in_specs = specs((OUTER, HEAD), TP)
    out_specs = P((OUTER, HEAD, TP), None)

    def run(*arrays):
        sequence, tensor = mesh.shape["sp"], mesh.shape["tp"]
        heads = arrays[14].shape[1] // tensor
        sizes = (arrays[0].shape[0] // sequence, arrays[13].shape[2], arrays[12].shape[2] // 2)
        reach = arrays[4].shape[0] // 2
        if (
            tensor == 2
            and heads > 1
            and sequence == 4 * heads
            and 2 * heads <= 8
            and sizes == (128, 256, 256)
            and arrays[5].shape[0] == heads * tensor * 128
            and arrays[0].shape[1] == sequence * 128
            and reach < 16
        ):
            grid = Mesh(mesh.devices.reshape(heads, 2, 2, tensor), AXES)
            rows = ("z", "y", "x")
            return jax.shard_map(
                near_shards,
                mesh=grid,
                in_specs=specs(rows, "tp"),
                out_specs=P(rows + ("tp",), None),
                check_vma=False,
            )(*arrays)
        parts = heads if sequence % heads == 0 else 1
        assert parts == heads
        fine = Mesh(mesh.devices.reshape(sequence // parts, parts, tensor), (OUTER, HEAD, TP))
        return jax.shard_map(
            shards, mesh=fine, in_specs=in_specs, out_specs=out_specs, check_vma=False
        )(*arrays)

    return run
```
